32 devices in a mesh: sp: 8 (over z, core), tp: 4 (over y, x).
Axes of the slice: x: 2, y: 2, z: 4, core: 2. Of those that a mesh axis runs over, the one named last changes fastest.
Arguments:
- b_gate: bfloat16 [2048, 1024], P('sp', 'tp'), may hold values from -6 to 6
- c_gate: bfloat16 [2048, 1024], P('sp', 'tp'), may hold values from -6 to 6
- h_in: bfloat16 [2048, 1024], P('sp', 'tp'), may hold values from -6 to 6
- docs: int32 [2048], replicated, may hold values from 0 to 3, never falling along the last dimension, each value on 1 to 1024 neighbouring positions
- conv_taps: bfloat16 [3, 1024], replicated, may hold values from -3 to 3
- out_weight: bfloat16 [1024, 4096], P(None, 'tp'), may hold values from -0.1875 to 0.1875
- residual_in: bfloat16 [2048, 4096], P('sp', 'tp'), may hold values from -52 to 52
- norm_gain: bfloat16 [4096], replicated, may hold values from 0.099609375 to 1.8984375
- expert_pick: int32 [2048, 2], P('sp'), may hold values from 0 to 7, as said below
- route_weight: float32 [2048, 2], P('sp'), may hold values from 0.5 to 2
- w_gate: bfloat16 [8, 4096, 2048], P('sp', None, 'tp'), may hold values from -0.09375 to 0.09375
- w_up: bfloat16 [8, 4096, 2048], P('sp', None, 'tp'), may hold values from -0.09375 to 0.09375
- w_down: bfloat16 [8, 2048, 4096], P('sp', None, 'tp'), may hold values from -0.125 to 0.125
Outputs:
- stream_out: bfloat16 [2048, 4096], P('sp', 'tp')
The draws below stay inside these ranges and needn't reach their ends.
Inputs may be any that keep to these rules, and one draw needn't show every extreme that they name: `expert_pick`: each row names 2 different experts of one group; group g holds experts g * 2 up to the next group's first.
All inputs are finite; a program needn't handle non-finite values.
Results may differ from the reference program's by a relative error of at most 0.012.
Values may be sent and summed in bfloat16 or wider, within the bound.
A program may use at most 64 MiB of HBM per device.

```python
import math
import jax
import jax.numpy as jnp
import numpy as np
from jax import lax

D = 4096
CH = 1024
FFE = 2048
GROUPS = 4
TOP_K = 2
TOK_DEV = 256
TOKENS = 2048
EXPERTS = 8
CAP = 80
N_SP = 8


def draw_expert_pick(key, part):
    per_group = EXPERTS // GROUPS
    key_group, key_first, key_second = jax.random.split(jax.random.fold_in(key, 11), 3)
    group_ids = jax.random.randint(key_group, (TOKENS,), 0, GROUPS)
    first_pick = jax.random.randint(key_first, (TOKENS,), 0, per_group)
    second_pick = (first_pick + jax.random.randint(key_second, (TOKENS,), 1, per_group)) % per_group
    return jnp.stack([group_ids * per_group + first_pick, group_ids * per_group + second_pick], axis=1).astype(jnp.int32)


def draw_residual_in(key, part):
    key_base, key_rows = jax.random.split(jax.random.fold_in(key, 23), 2)
    column_scale = jnp.exp(jnp.linspace(math.log(0.3), math.log(3.0), D)).astype(jnp.float32)
    row_scale = jnp.exp(jax.random.uniform(key_rows, (TOKENS, 1), jnp.float32, math.log(0.4), math.log(4.0)))
    base = jnp.clip(jax.random.normal(key_base, (TOKENS, D), jnp.float32), -4.0, 4.0)
    return (base * row_scale * column_scale[None, :]).astype(jnp.bfloat16)


def level_of(key, extent, cuts, low, largest):
    def one(axis_at, shards_of):
        draws = jax.random.uniform(jax.random.fold_in(jax.random.fold_in(key, 6), axis_at), (shards_of,), jnp.float32, low / len(cuts), largest / len(cuts))
        return jnp.repeat(jnp.exp(draws), extent[axis_at] // shards_of).reshape((-1,) + (1,) * (len(extent) - axis_at - 1))

    factor_of = one(*cuts[0])
    for cut in cuts[1:]:
        factor_of = factor_of * one(*cut)
    return factor_of


def profile(amount, total, reach, skew):
    weights = [(1 << 20) // math.isqrt(standing ** skew) + 1 for standing in range(2, amount + 1)]
    spare, counts = total - reach - (amount - 1), [1] * (amount - 1)
    while spare > 0:
        candidates = [i for i in range(amount - 1) if counts[i] < reach]
        mass, budget = sum([weights[i] for i in candidates]), spare
        for i in candidates:
            extra = min(reach - counts[i], max(1, budget * weights[i] // mass), spare)
            counts[i] = counts[i] + extra
            spare = spare - extra
    return np.array([reach] + counts)


def uneven_parts(rng, count, total, most, lean):
    if count == 2:
        one = jax.random.randint(rng, (), max(1, total - most), min(most, total - 1) + 1)
        return jnp.stack([one, total - one])
    sizes = jnp.asarray(profile(count, total, most, lean), jnp.int32)
    couples = (count - 1) // 2
    giver, sink = sizes[1:1 + 2 * couples:2], sizes[2:2 + 2 * couples:2]
    margin = jnp.minimum(giver - 1, most - sink)
    passed = jax.random.randint(jax.random.fold_in(rng, 1), (couples,), 0, 1 << 20) % (margin + 1)
    sizes = sizes.at[1:1 + 2 * couples:2].set(giver - passed).at[2:2 + 2 * couples:2].set(sink + passed)
    return sizes[jax.random.permutation(jax.random.fold_in(rng, 2), count)]


def normal_values(stream_key, dims, scale, most, cuts=(), held_as=jnp.bfloat16):
    loudness = level_of(stream_key, dims, cuts, -0.22, 0.18) if cuts else 1.0
    values = jax.random.normal(stream_key, dims, jnp.float32) * scale * loudness
    return jnp.minimum(jnp.maximum(values, -most), most).astype(held_as)


def setup_inputs(seed: int = 0) -> dict:
    splits = jax.random.split(jax.random.key(seed), 14)
    b_gate = normal_values(splits[0], (TOKENS, CH), 1.0, 6.0, ((0, 8), (1, 4)))
    c_gate = normal_values(splits[1], (TOKENS, CH), 1.0, 6.0, ((0, 8), (1, 4)))
    h_in = normal_values(splits[2], (TOKENS, CH), 1.0, 6.0, ((0, 8), (1, 4)))
    docs = jnp.searchsorted(jnp.cumsum(uneven_parts(splits[3], N_SP // 2, TOKENS, 4 * TOK_DEV, 1)), jnp.arange(TOKENS), side="right").astype(jnp.int32)
    conv_taps = normal_values(splits[4], (3, CH), 0.577, 3.0)
    out_weight = normal_values(splits[5], (CH, D), CH ** -0.5, 0.1875, ((1, 4),))
    residual_in = draw_residual_in(jax.random.fold_in(splits[13], 71), 0)
    norm_gain = jnp.clip(1.0 + 0.18 * jax.random.normal(splits[7], (D,), jnp.float32), 0.099609375, 1.8984375).astype(jnp.bfloat16)
    expert_pick = draw_expert_pick(jax.random.fold_in(splits[13], 71), 0)
    route_weight = jnp.clip(jnp.exp(math.log(2.0) - 1.3862944 * jax.random.uniform(splits[9], (TOKENS, TOP_K), jnp.float32) ** level_of(splits[9], (TOKENS, TOP_K), ((0, 8),), -0.2, 0.2)), 0.5, 2.0)
    w_gate = normal_values(splits[10], (EXPERTS, D, FFE), D ** -0.5, 0.09375, ((0, 8), (2, 4)))
    w_up = normal_values(splits[11], (EXPERTS, D, FFE), D ** -0.5, 0.09375, ((0, 8), (2, 4)))
    w_down = normal_values(splits[12], (EXPERTS, FFE, D), FFE ** -0.5, 0.125, ((0, 8), (2, 4)))
    return {"b_gate": b_gate, "c_gate": c_gate, "h_in": h_in, "docs": docs, "conv_taps": conv_taps, "out_weight": out_weight, "residual_in": residual_in, "norm_gain": norm_gain, "expert_pick": expert_pick, "route_weight": route_weight, "w_gate": w_gate, "w_up": w_up, "w_down": w_down}


NORM_EPS = 1e-06

def reference(b_gate, c_gate, h_in, docs, conv_taps, out_weight, residual_in, norm_gain, expert_pick, route_weight, w_gate, w_up, w_down):
    product = (c_gate.astype(jnp.float32) * h_in.astype(jnp.float32)).astype(jnp.bfloat16)
    product_f = product.astype(jnp.float32)
    tap_weights = conv_taps.astype(jnp.float32)
    conv_sum = tap_weights[0][None, :] * product_f
    for step_back in (1, 2):
        earlier = jnp.concatenate([jnp.zeros((step_back, CH), jnp.float32), product_f[:-step_back]], axis=0)
        earlier_doc = jnp.concatenate([jnp.full((step_back,), -1, jnp.int32), docs[:-step_back]], axis=0)
        same_doc = (earlier_doc == docs).astype(jnp.float32)[:, None]
        conv_sum = conv_sum + tap_weights[step_back][None, :] * earlier * same_doc
    conv_out = (b_gate.astype(jnp.float32) * conv_sum).astype(jnp.bfloat16)
    stream = (residual_in.astype(jnp.float32) + jnp.dot(conv_out, out_weight, preferred_element_type=jnp.float32)).astype(jnp.bfloat16)
    stream_f = stream.astype(jnp.float32)
    inverse = lax.rsqrt(lax.optimization_barrier(jnp.mean(stream_f * stream_f, axis=1, keepdims=True)) + NORM_EPS)
    normed = (stream_f * inverse * norm_gain.astype(jnp.float32)[None, :]).astype(jnp.bfloat16)
    per_block = expert_pick.reshape(N_SP, TOK_DEV * TOP_K)
    onehot = (per_block[:, :, None] == jnp.arange(EXPERTS, dtype=jnp.int32)[None, None, :]).astype(jnp.int32)
    slot_pos = lax.optimization_barrier(jnp.sum((jnp.cumsum(onehot, axis=1) - onehot) * onehot, axis=2))
    kept_mask = slot_pos < CAP
    block_ids = jnp.arange(N_SP, dtype=jnp.int32)[:, None]
    target = (per_block * N_SP + block_ids) * CAP + jnp.minimum(slot_pos, CAP - 1)
    target = jnp.where(kept_mask, target, EXPERTS * N_SP * CAP).astype(jnp.int32)
    assign_ids = jnp.arange(N_SP * TOK_DEV * TOP_K, dtype=jnp.int32).reshape(N_SP, TOK_DEV * TOP_K)
    table = jnp.full((EXPERTS * N_SP * CAP + 1,), -1, jnp.int32).at[target.reshape(-1)].set(assign_ids.reshape(-1))
    table = table[:-1].reshape(EXPERTS, N_SP * CAP)
    weights_flat = route_weight.reshape(-1)

    def one_expert(running, expert):
        sources = table[expert]
        filled = sources >= 0
        safe_ids = jnp.maximum(sources, 0)
        token_ids = safe_ids // TOP_K
        inputs = jnp.where(filled[:, None], normed[token_ids], jnp.zeros((), normed.dtype))
        gate_pre = jnp.dot(inputs, w_gate[expert], preferred_element_type=jnp.float32)
        up_pre = jnp.dot(inputs, w_up[expert], preferred_element_type=jnp.float32)
        hidden = (jax.nn.silu(gate_pre) * up_pre).astype(jnp.bfloat16)
        result = jnp.dot(hidden, w_down[expert], preferred_element_type=jnp.float32).astype(jnp.bfloat16)
        factor = jnp.where(filled, weights_flat[safe_ids], jnp.zeros((), weights_flat.dtype))
        scaled = result.astype(jnp.float32) * factor[:, None]
        return (running.at[token_ids].add(scaled), None)
    feed_out, unused = lax.scan(one_expert, jnp.zeros((TOKENS, D), jnp.float32), jnp.arange(EXPERTS, dtype=jnp.int32))
    return (stream_f + feed_out).astype(jnp.bfloat16)
```

```python
import functools

import jax
import jax.numpy as jnp
from jax import lax
from jax.experimental import pallas as pl
from jax.experimental.pallas import tpu as pltpu
from jax.sharding import PartitionSpec as P

TOP_K = 2
GROUPS = 4
MESH = pl.DeviceIdType.MESH


NORM_EPS = 1e-06


def passed_along(value, axis, steps):
    count = lax.axis_size(axis)
    first, last = (max(0, -steps), min(count, count - steps))
    return lax.ppermute(value, axis, [(source, source + steps) for source in range(first, last)])


def general(
    b_gate,
    c_gate,
    h_in,
    docs,
    conv_taps,
    out_weight,
    residual_in,
    norm_gain,
    expert_pick,
    route_weight,
    w_gate,
    w_up,
    w_down,
):
    tok_rows, local_chans = h_in.shape
    width = residual_in.shape[1]
    full_dim = w_gate.shape[1]
    n_sp = lax.axis_size("sp")
    sp_index = lax.axis_index("sp")
    tp_index = lax.axis_index("tp")
    first_pos = sp_index * tok_rows
    product = (c_gate.astype(jnp.float32) * h_in.astype(jnp.float32)).astype(jnp.bfloat16)
    edge = passed_along(product[tok_rows - 2 :], "sp", 1)
    extended = jnp.concatenate([edge, product], axis=0).astype(jnp.float32)
    own_docs = lax.dynamic_slice_in_dim(docs, first_pos, tok_rows)
    padded_docs = jnp.concatenate([jnp.full((2,), -1, jnp.int32), docs], axis=0)
    near_docs = lax.dynamic_slice_in_dim(padded_docs, first_pos, tok_rows + 2)
    tap_weights = lax.dynamic_slice_in_dim(
        conv_taps, tp_index * local_chans, local_chans, 1
    ).astype(jnp.float32)
    conv_sum = tap_weights[0][None, :] * extended[2:]
    for step_back in (1, 2):
        same_doc = (near_docs[2 - step_back : 2 - step_back + tok_rows] == own_docs).astype(
            jnp.float32
        )[:, None]
        conv_sum = (
            conv_sum
            + tap_weights[step_back][None, :]
            * extended[2 - step_back : 2 - step_back + tok_rows]
            * same_doc
        )
    conv_out = (b_gate.astype(jnp.float32) * conv_sum).astype(jnp.bfloat16)
    projected = jnp.dot(
        lax.all_gather(conv_out, "tp", axis=1, tiled=True),
        out_weight,
        preferred_element_type=jnp.float32,
    )
    stream = (residual_in.astype(jnp.float32) + projected).astype(jnp.bfloat16)
    stream_f = stream.astype(jnp.float32)
    capacity = 5 * tok_rows // (2 * n_sp)
    assign_flat = expert_pick.reshape(-1)
    onehot = (assign_flat[:, None] == jnp.arange(n_sp, dtype=jnp.int32)[None, :]).astype(jnp.int32)
    slot_pos = jnp.sum((jnp.cumsum(onehot, axis=0) - onehot) * onehot, axis=1)
    kept_mask = slot_pos < capacity
    target = jnp.where(
        kept_mask, assign_flat * capacity + jnp.minimum(slot_pos, capacity - 1), n_sp * capacity
    )
    table = (
        jnp.full((n_sp * capacity + 1,), -1, jnp.int32)
        .at[target]
        .set(jnp.arange(assign_flat.shape[0], dtype=jnp.int32))[:-1]
    )
    filled = table >= 0
    source_rows = jnp.maximum(table, 0) // TOP_K
    gate_local = w_gate[0]
    up_local = w_up[0]
    slot_rows = n_sp * capacity
    squares = lax.psum(jnp.sum(stream_f * stream_f, axis=1), "tp")
    inverse = lax.rsqrt(squares / full_dim + NORM_EPS)[:, None]
    gain_cols = lax.dynamic_slice_in_dim(norm_gain, tp_index * width, width).astype(jnp.float32)
    normed = (stream_f * inverse * gain_cols[None, :]).astype(jnp.bfloat16)
    outgoing = jnp.where(filled[:, None], normed[source_rows], jnp.zeros((), normed.dtype)).reshape(
        n_sp, capacity, width
    )
    received = lax.all_to_all(outgoing, "sp", split_axis=0, concat_axis=0, tiled=True)
    shard_piece = lax.all_gather(received, "tp", axis=2, tiled=True)
    flat_piece = shard_piece.reshape(slot_rows, shard_piece.shape[2])
    gate_pre = jnp.dot(flat_piece, gate_local, preferred_element_type=jnp.float32)
    up_pre = jnp.dot(flat_piece, up_local, preferred_element_type=jnp.float32)
    hidden = (jax.nn.silu(gate_pre) * up_pre).astype(jnp.bfloat16)
    down_local = w_down[0]
    result = jnp.dot(
        lax.all_gather(hidden, "tp", axis=1, tiled=True),
        down_local,
        preferred_element_type=jnp.float32,
    ).astype(jnp.bfloat16)
    returned = lax.all_to_all(
        result.reshape(n_sp, capacity, width), "sp", split_axis=0, concat_axis=0, tiled=True
    ).reshape(n_sp * capacity, width)
    picked = jnp.where(
        kept_mask[:, None],
        returned[jnp.minimum(target, n_sp * capacity - 1)].astype(jnp.float32),
        0.0,
    )
    weighted = picked * route_weight.reshape(-1)[:, None]
    feed_out = jnp.sum(weighted.reshape(tok_rows, TOP_K, width), axis=1)
    return (stream_f + feed_out).astype(jnp.bfloat16)


def flipped(index, mask):
    bit = 1
    while bit <= mask:
        if mask & bit:
            index = index + bit * (1 - 2 * ((index // bit) % 2))
        bit *= 2
    return index


def fused_kernel(
    n_chips,
    capacity,
    b_ref,
    c_ref,
    h_ref,
    cols_ref,
    taps_ref,
    resid_ref,
    gain_ref,
    ow_hbm,
    wg_hbm,
    wu_hbm,
    wd_hbm,
    out_ref,
    ow,
    wg,
    wu,
    wd,
    ext,
    cv,
    stream,
    acc,
    pt,
    rows_out,
    wts_out,
    rows,
    wts,
    normed,
    hid,
    e_own,
    e_send,
    e_recv,
    feed_out,
    back,
    local_sems,
    send_sems,
    recv_sems,
):
    tok_rows, chans = h_ref.shape
    width = resid_ref.shape[1]
    full = gain_ref.shape[1]
    hid_cols = wg.shape[1]
    sp = lax.axis_index("sp")
    tp = lax.axis_index("tp")
    chip = sp // 2
    core = sp % 2
    tp_x = (tp // 2) * 2 + (1 - tp % 2)
    tp_y = (1 - tp // 2) * 2 + tp % 2
    tp_d = (1 - tp // 2) * 2 + (1 - tp % 2)
    dev_x = (sp, tp_x)
    dev_y = (sp, tp_y)
    dev_s = (chip * 2 + (1 - core), tp)
    ks = list(range(n_chips))
    dev_z = [(flipped(chip, k) * 2 + core, tp) for k in ks]

    loads = []
    for i, (s, d) in enumerate(((ow_hbm, ow), (wg_hbm.at[0], wg), (wu_hbm.at[0], wu), (wd_hbm.at[0], wd))):
        cp = pltpu.make_async_copy(s, d, local_sems.at[i])
        cp.start()
        loads.append(cp)

    count = [0]
    sent = []

    def remote(s, d, dev):
        i = count[0]
        count[0] += 1
        return pltpu.make_async_remote_copy(
            src_ref=s, dst_ref=d, send_sem=send_sems.at[i], recv_sem=recv_sems.at[i],
            device_id=dev, device_id_type=MESH,
        )

    def go(s, d, dev):
        cp = remote(s, d, dev)
        cp.start()
        sent.append(cp)
        return cp

    def cols(index, size):
        return pl.ds(pl.multiple_of(index * size, 128), size)

    barrier = pltpu.get_barrier_semaphore()
    peers = [dev_x, dev_y, dev_s] + dev_z[1:]
    for dev in peers:
        pl.semaphore_signal(barrier, inc=1, device_id=dev, device_id_type=MESH)
    other = jnp.where(core == 0, sp - 1, sp + 1)
    has_other = jnp.where(core == 0, chip > 0, chip < n_chips - 1)

    @pl.when(has_other)
    def _():
        pl.semaphore_signal(barrier, inc=1, device_id=(other, tp), device_id_type=MESH)

    product = (c_ref[...].astype(jnp.float32) * h_ref[...].astype(jnp.float32)).astype(jnp.bfloat16)
    ext[8:, :] = product.astype(jnp.float32)
    pl.semaphore_wait(barrier, len(peers) + has_other.astype(jnp.int32))

    edge = remote(ext.at[pl.ds(tok_rows, 8)], ext.at[pl.ds(0, 8)], (sp + 1, tp))

    @pl.when(sp < 2 * n_chips - 1)
    def _():
        edge.start()

    lane = lax.broadcasted_iota(jnp.int32, (tok_rows, 128), 1)
    lane_f = lane.astype(jnp.float32)
    group = cols_ref[:, 2:3]
    onehot = (group == lane_f).astype(jnp.float32)
    earlier = (
        lax.broadcasted_iota(jnp.int32, (tok_rows, tok_rows), 1)
        < lax.broadcasted_iota(jnp.int32, (tok_rows, tok_rows), 0)
    ).astype(jnp.float32).astype(jnp.bfloat16)
    before = jnp.dot(earlier, onehot.astype(jnp.bfloat16), preferred_element_type=jnp.float32)
    slot = jnp.sum(before * onehot, axis=1, keepdims=True)
    for k in ks:
        here = flipped(chip, k).astype(jnp.float32)
        hit = jnp.where((group == here) & (slot == lane_f) & (lane < capacity), 1.0, 0.0)
        pt[k] = hit.astype(jnp.bfloat16)
    parts = jnp.zeros((tok_rows, 128), jnp.float32)
    for j in range(2):
        w = cols_ref[:, 3 + j : 4 + j]
        for i in range(3):
            piece = w.astype(jnp.bfloat16).astype(jnp.float32)
            parts = jnp.where(lane == 3 * j + i, piece, parts)
            w = w - piece
    parts = parts.astype(jnp.bfloat16)
    for k in ks:
        got = lax.dot_general(
            pt[k], parts, (((0,), (0,)), ((), ())), preferred_element_type=jnp.float32
        )
        wts_out[k] = got[:capacity].astype(jnp.bfloat16)
    wts[0] = wts_out[0]

    @pl.when(sp > 0)
    def _():
        edge.wait_recv()

    @pl.when(sp == 0)
    def _():
        ext[0:8, :] = jnp.zeros((8, chans), jnp.float32)

    taps = taps_ref[:, cols(tp, chans)].astype(jnp.float32)
    conv = taps[0:1, :] * ext[8 : 8 + tok_rows, :]
    for lag in (1, 2):
        conv = conv + taps[lag : lag + 1, :] * ext[8 - lag : 8 - lag + tok_rows, :] * cols_ref[:, lag - 1 : lag]
    conv = (b_ref[...].astype(jnp.float32) * conv).astype(jnp.bfloat16)
    cv[:, cols(tp, chans)] = conv

    def spread(buf, size, own_sends):
        mine = buf.at[:, cols(tp, size)]
        own_sends.append(go(mine, mine, dev_x))
        own_sends.append(go(mine, mine, dev_y))

    def relay(buf, size, sends):
        half = size // 2
        sends[1].wait_recv()
        part = buf.at[:, cols(tp_y * 2, half)]
        sends.append(go(part, part, dev_x))
        sends[0].wait_recv()
        part = buf.at[:, cols(tp_x * 2 + 1, half)]
        sends.append(go(part, part, dev_y))

    conv_sends = []
    spread(cv, chans, conv_sends)

    def proj(index):
        rows_ = pl.ds(pl.multiple_of(index * chans, 128), chans)
        return jnp.dot(cv[:, cols(index, chans)], ow[rows_, :], preferred_element_type=jnp.float32)

    loads[0].wait()
    acc[...] = resid_ref[...].astype(jnp.float32) + proj(tp)
    relay(cv, chans, conv_sends)
    acc[...] += proj(tp_x)
    acc[...] += proj(tp_y)
    conv_sends[2].wait_recv()
    conv_sends[3].wait_recv()
    stream[...] = (acc[...] + proj(tp_d)).astype(jnp.bfloat16)

    z_rows, z_wts = [None] * n_chips, [None] * n_chips
    mine = cols(tp, width)
    for k in [0] + ks[1:]:
        got = lax.dot_general(
            pt[k], stream[...], (((0,), (0,)), ((), ())), preferred_element_type=jnp.float32
        )[:capacity].astype(jnp.bfloat16)
        if k == 0:
            rows[0, 0, :, mine] = got
        else:
            rows_out[k] = got
            z_rows[k] = go(rows_out.at[k], rows.at[k, 0, :, mine], dev_z[k])
        if k == 0:
            row_sends = [[] for _ in ks]
            sis = [[] for _ in ks]
            first = True
            spread(rows.at[0, 0], width, row_sends[0])
            sis[0].append(go(rows.at[0, 0, :, mine], rows.at[0, 1, :, mine], dev_s))
    for k in ks[1:]:
        z_wts[k] = go(wts_out.at[k], wts.at[k], dev_z[k])

    def share(k, index, size):
        at = cols(index, size)
        sis[k].append(go(rows.at[k, 0, :, at], rows.at[k, 1, :, at], dev_s))

    def stage(k):
        if k > 0:
            z_rows[k].wait_recv()
            spread(rows.at[k, 0], width, row_sends[k])
            share(k, tp, width)

    def forward(k):
        relay(rows.at[k, 0], width, row_sends[k])
        share(k, tp_x, width)
        share(k, tp_y, width)

    def finish(k):
        row_sends[k][2].wait_recv()
        share(k, tp_d * 2, width // 2)
        row_sends[k][3].wait_recv()
        share(k, tp_d * 2 + 1, width // 2)

    hid_sends = [[] for _ in ks]

    def expand(k):
        for cp in sis[k]:
            cp.wait_recv()
        for p in range(2):
            def norm(r, carry, p=p):
                at = pl.ds(pl.multiple_of(r * 16, 16), 16)
                x = rows[k, p, at, :].astype(jnp.float32)
                ms = jnp.sum(x * x, axis=1, keepdims=True) / full
                inv = lax.rsqrt(ms + NORM_EPS)
                y = (x * inv * gain_ref[...]).astype(jnp.bfloat16)
                normed[pl.ds(pl.multiple_of(p * capacity + r * 16, 16), 16), :] = y
                return carry
            lax.fori_loop(0, capacity // 16, norm, 0)
        if k == 0:
            loads[1].wait()
            loads[2].wait()

        def tile(n, carry):
            at = pl.ds(pl.multiple_of(n * 256, 256), 256)
            x = normed[...]
            g = jnp.dot(x, wg[:, at], preferred_element_type=jnp.float32)
            u = jnp.dot(x, wu[:, at], preferred_element_type=jnp.float32)
            h = (g / (1.0 + jnp.exp(-g)) * u).astype(jnp.bfloat16)
            hid[k, :, pl.ds(pl.multiple_of(tp * hid_cols + n * 256, 256), 256)] = h
            return carry

        lax.fori_loop(0, hid_cols // 256, tile, 0)
        spread(hid.at[k], hid_cols, hid_sends[k])

    def hid_forward(k):
        relay(hid.at[k], hid_cols, hid_sends[k])

    e_sends = [None] * n_chips
    z_back = [None] * n_chips

    def down(k):
        hid_sends[k][2].wait_recv()
        hid_sends[k][3].wait_recv()
        if k == 0:
            loads[3].wait()

        def tile(n, carry):
            at = pl.ds(pl.multiple_of(n * 256, 256), 256)
            e = jnp.dot(hid[k], wd[:, at], preferred_element_type=jnp.float32).astype(jnp.bfloat16)
            e_own[k, :, at] = e[:capacity]
            e_send[k, :, at] = e[capacity:]
            return carry

        lax.fori_loop(0, width // 256, tile, 0)
        e_sends[k] = go(e_send.at[k], e_recv.at[k], dev_s)

    def combine(k):
        if k > 0:
            z_wts[k].wait_recv()
        w = wts[k].astype(jnp.float32)
        w_lane = lax.broadcasted_iota(jnp.int32, w.shape, 1)
        w_even = jnp.sum(jnp.where(w_lane < 3, w, 0.0), axis=1, keepdims=True)
        w_odd = jnp.sum(jnp.where((w_lane >= 3) & (w_lane < 6), w, 0.0), axis=1, keepdims=True)
        pick = core.astype(jnp.float32)
        w_mine = w_even * (1.0 - pick) + w_odd * pick
        w_other = w_odd * (1.0 - pick) + w_even * pick
        e_sends[k].wait_recv()
        f = (e_own[k].astype(jnp.float32) * w_mine + e_recv[k].astype(jnp.float32) * w_other).astype(jnp.bfloat16)
        if k == 0:
            back[0, 0:capacity, :] = f
        else:
            feed_out[k] = f
            z_back[k] = go(feed_out.at[k], back.at[k, pl.ds(0, capacity), :], dev_z[k])

    for k in ks:
        back[k, capacity:, :] = jnp.zeros((128 - capacity, width), jnp.bfloat16)

    last = n_chips - 1
    plan = sorted(
        [(3 * k, 0, stage, k) for k in ks]
        + [(3 * k + 4, 1, forward, k) for k in ks]
        + [(3 * k + 7, 2, finish, k) for k in ks]
        + [(3 * k + 9, 3, expand, k) for k in ks]
        + [(3 * k + 13, 4, hid_forward, k) for k in ks]
        + [(3 * k + 16, 5, down, k) for k in ks]
        + [(3 * k + 18, 6, combine, k) for k in ks],
        key=lambda item: item[:2],
    )
    for _, _, step, k in plan:
        step(k)

    acc[...] = stream[...].astype(jnp.float32)
    for k in ks:
        if k > 0:
            z_back[k].wait_recv()
        acc[...] += jnp.dot(pt[k], back[k], preferred_element_type=jnp.float32)
    out_ref[...] = acc[...].astype(jnp.bfloat16)

    for cp in sent:
        cp.wait_send()

    @pl.when(sp < 2 * n_chips - 1)
    def _():
        edge.wait_send()


def fused(
    b_gate,
    c_gate,
    h_in,
    docs,
    conv_taps,
    out_weight,
    residual_in,
    norm_gain,
    expert_pick,
    route_weight,
    w_gate,
    w_up,
    w_down,
):
    tok_rows, chans = h_in.shape
    width = residual_in.shape[1]
    full = w_gate.shape[1]
    hid_cols = w_gate.shape[2]
    hid_full = w_down.shape[1]
    n_sp = lax.axis_size("sp")
    n_chips = n_sp // 2
    capacity = 5 * tok_rows // (2 * n_sp)
    first_pos = lax.axis_index("sp") * tok_rows
    padded_docs = jnp.concatenate([jnp.full((2,), -1, jnp.int32), docs], axis=0)
    near = lax.dynamic_slice_in_dim(padded_docs, first_pos, tok_rows + 2)
    own = near[2:]
    even = expert_pick[:, 0] % 2 == 0
    side = jnp.stack(
        [
            (near[1:-1] == own).astype(jnp.float32),
            (near[:-2] == own).astype(jnp.float32),
            (expert_pick[:, 0] // 2).astype(jnp.float32),
            jnp.where(even, route_weight[:, 0], route_weight[:, 1]),
            jnp.where(even, route_weight[:, 1], route_weight[:, 0]),
        ],
        axis=1,
    )
    gain = norm_gain.astype(jnp.float32)[None, :]
    n_copies = 5 + 2 * (n_chips - 1) + 14 * n_chips + n_chips - 1
    vmem = pl.BlockSpec(memory_space=pltpu.VMEM)
    hbm = pl.BlockSpec(memory_space=pl.ANY)
    bf16 = jnp.bfloat16
    return pl.pallas_call(
        functools.partial(fused_kernel, n_chips, capacity),
        out_shape=jax.ShapeDtypeStruct((tok_rows, width), bf16),
        in_specs=[vmem] * 7 + [hbm] * 4,
        out_specs=vmem,
        scratch_shapes=[
            pltpu.VMEM(out_weight.shape, bf16),
            pltpu.VMEM(w_gate.shape[1:], bf16),
            pltpu.VMEM(w_up.shape[1:], bf16),
            pltpu.VMEM(w_down.shape[1:], bf16),
            pltpu.VMEM((tok_rows + 8, chans), jnp.float32),
            pltpu.VMEM((tok_rows, out_weight.shape[0]), bf16),
            pltpu.VMEM((tok_rows, width), bf16),
            pltpu.VMEM((tok_rows, width), jnp.float32),
            pltpu.VMEM((n_chips, tok_rows, 128), bf16),
            pltpu.VMEM((n_chips, capacity, width), bf16),
            pltpu.VMEM((n_chips, capacity, 128), bf16),
            pltpu.VMEM((n_chips, 2, capacity, full), bf16),
            pltpu.VMEM((n_chips, capacity, 128), bf16),
            pltpu.VMEM((2 * capacity, full), bf16),
            pltpu.VMEM((n_chips, 2 * capacity, hid_full), bf16),
            pltpu.VMEM((n_chips, capacity, width), bf16),
            pltpu.VMEM((n_chips, capacity, width), bf16),
            pltpu.VMEM((n_chips, capacity, width), bf16),
            pltpu.VMEM((n_chips, capacity, width), bf16),
            pltpu.VMEM((n_chips, 128, width), bf16),
            pltpu.SemaphoreType.DMA((4,)),
            pltpu.SemaphoreType.DMA((n_copies,)),
            pltpu.SemaphoreType.DMA((n_copies,)),
        ],
        compiler_params=pltpu.CompilerParams(
            collective_id=0, has_side_effects=True, vmem_limit_bytes=56 * 1024 * 1024
        ),
    )(b_gate, c_gate, h_in, side, conv_taps, residual_in, gain, out_weight, w_gate, w_up, w_down)


def pairs_fit(mesh):
    n_sp, n_tp = mesh.shape["sp"], mesh.shape["tp"]
    return n_sp == GROUPS * TOP_K and TOP_K == 2 and n_tp == 4


def solution(mesh):
    return jax.shard_map(
        fused if pairs_fit(mesh) else general,
        mesh=mesh,
        in_specs=(
            P("sp", "tp"),
            P("sp", "tp"),
            P("sp", "tp"),
            P(),
            P(),
            P(None, "tp"),
            P("sp", "tp"),
            P(),
            P("sp", None),
            P("sp", None),
            P("sp", None, "tp"),
            P("sp", None, "tp"),
            P("sp", None, "tp"),
        ),
        out_specs=P("sp", "tp"),
        check_vma=False,
    )
```

```python
import functools

import jax
import jax.numpy as jnp
from jax import lax
from jax.experimental import pallas as pl
from jax.experimental.pallas import tpu as pltpu
from jax.sharding import PartitionSpec as P

TOP_K = 2
GROUPS = 4
PLAN = (
    "S1 F0 S2 F1 S3 D0 E0 F2 D1 E1 X1 F3 D2 E2 X2 R1 D3 E3 X3 "
    "R2 W1 C1 R3 X0 W2 W3 C2 C3 R0 W0 C0"
)
FINAL = (1, 0, 2, 3)
MESH = pl.DeviceIdType.MESH


NORM_EPS = 1e-06


def passed_along(value, axis, steps):
    count = lax.axis_size(axis)
    first, last = (max(0, -steps), min(count, count - steps))
    return lax.ppermute(value, axis, [(source, source + steps) for source in range(first, last)])


def general(
    b_gate,
    c_gate,
    h_in,
    docs,
    conv_taps,
    out_weight,
    residual_in,
    norm_gain,
    expert_pick,
    route_weight,
    w_gate,
    w_up,
    w_down,
):
    tok_rows, local_chans = h_in.shape
    width = residual_in.shape[1]
    full_dim = w_gate.shape[1]
    n_sp = lax.axis_size("sp")
    sp_index = lax.axis_index("sp")
    tp_index = lax.axis_index("tp")
    first_pos = sp_index * tok_rows
    product = (c_gate.astype(jnp.float32) * h_in.astype(jnp.float32)).astype(jnp.bfloat16)
    edge = passed_along(product[tok_rows - 2 :], "sp", 1)
    extended = jnp.concatenate([edge, product], axis=0).astype(jnp.float32)
    own_docs = lax.dynamic_slice_in_dim(docs, first_pos, tok_rows)
    padded_docs = jnp.concatenate([jnp.full((2,), -1, jnp.int32), docs], axis=0)
    near_docs = lax.dynamic_slice_in_dim(padded_docs, first_pos, tok_rows + 2)
    tap_weights = lax.dynamic_slice_in_dim(
        conv_taps, tp_index * local_chans, local_chans, 1
    ).astype(jnp.float32)
    conv_sum = tap_weights[0][None, :] * extended[2:]
    for step_back in (1, 2):
        same_doc = (near_docs[2 - step_back : 2 - step_back + tok_rows] == own_docs).astype(
            jnp.float32
        )[:, None]
        conv_sum = (
            conv_sum
            + tap_weights[step_back][None, :]
            * extended[2 - step_back : 2 - step_back + tok_rows]
            * same_doc
        )
    conv_out = (b_gate.astype(jnp.float32) * conv_sum).astype(jnp.bfloat16)
    projected = jnp.dot(
        lax.all_gather(conv_out, "tp", axis=1, tiled=True),
        out_weight,
        preferred_element_type=jnp.float32,
    )
    stream = (residual_in.astype(jnp.float32) + projected).astype(jnp.bfloat16)
    stream_f = stream.astype(jnp.float32)
    capacity = 5 * tok_rows // (2 * n_sp)
    assign_flat = expert_pick.reshape(-1)
    onehot = (assign_flat[:, None] == jnp.arange(n_sp, dtype=jnp.int32)[None, :]).astype(jnp.int32)
    slot_pos = jnp.sum((jnp.cumsum(onehot, axis=0) - onehot) * onehot, axis=1)
    kept_mask = slot_pos < capacity
    target = jnp.where(
        kept_mask, assign_flat * capacity + jnp.minimum(slot_pos, capacity - 1), n_sp * capacity
    )
    table = (
        jnp.full((n_sp * capacity + 1,), -1, jnp.int32)
        .at[target]
        .set(jnp.arange(assign_flat.shape[0], dtype=jnp.int32))[:-1]
    )
    filled = table >= 0
    source_rows = jnp.maximum(table, 0) // TOP_K
    gate_local = w_gate[0]
    up_local = w_up[0]
    slot_rows = n_sp * capacity
    squares = lax.psum(jnp.sum(stream_f * stream_f, axis=1), "tp")
    inverse = lax.rsqrt(squares / full_dim + NORM_EPS)[:, None]
    gain_cols = lax.dynamic_slice_in_dim(norm_gain, tp_index * width, width).astype(jnp.float32)
    normed = (stream_f * inverse * gain_cols[None, :]).astype(jnp.bfloat16)
    outgoing = jnp.where(filled[:, None], normed[source_rows], jnp.zeros((), normed.dtype)).reshape(
        n_sp, capacity, width
    )
    received = lax.all_to_all(outgoing, "sp", split_axis=0, concat_axis=0, tiled=True)
    shard_piece = lax.all_gather(received, "tp", axis=2, tiled=True)
    flat_piece = shard_piece.reshape(slot_rows, shard_piece.shape[2])
    gate_pre = jnp.dot(flat_piece, gate_local, preferred_element_type=jnp.float32)
    up_pre = jnp.dot(flat_piece, up_local, preferred_element_type=jnp.float32)
    hidden = (jax.nn.silu(gate_pre) * up_pre).astype(jnp.bfloat16)
    down_local = w_down[0]
    result = jnp.dot(
        lax.all_gather(hidden, "tp", axis=1, tiled=True),
        down_local,
        preferred_element_type=jnp.float32,
    ).astype(jnp.bfloat16)
    returned = lax.all_to_all(
        result.reshape(n_sp, capacity, width), "sp", split_axis=0, concat_axis=0, tiled=True
    ).reshape(n_sp * capacity, width)
    picked = jnp.where(
        kept_mask[:, None],
        returned[jnp.minimum(target, n_sp * capacity - 1)].astype(jnp.float32),
        0.0,
    )
    weighted = picked * route_weight.reshape(-1)[:, None]
    feed_out = jnp.sum(weighted.reshape(tok_rows, TOP_K, width), axis=1)
    return (stream_f + feed_out).astype(jnp.bfloat16)


def flipped(index, mask):
    bit = 1
    while bit <= mask:
        if mask & bit:
            index = index + bit * (1 - 2 * ((index // bit) % 2))
        bit *= 2
    return index


def fused_kernel(
    n_chips,
    capacity,
    b_ref,
    c_ref,
    h_ref,
    docs_ref,
    pick_ref,
    weight_ref,
    taps_ref,
    gain_ref,
    resid_hbm,
    ow_hbm,
    wg_hbm,
    wu_hbm,
    wd_hbm,
    out_ref,
    resid,
    gain,
    ow,
    wg,
    wu,
    wd,
    ext,
    cv,
    stream,
    acc,
    pt,
    rows_out,
    wts_out,
    rows,
    wts,
    normed,
    hid,
    e_own,
    e_send,
    e_recv,
    feed_out,
    back,
    local_sems,
    send_sems,
    recv_sems,
):
    tok_rows, chans = h_ref.shape
    width = resid.shape[1]
    full = gain_ref.shape[0]
    hid_cols = wg.shape[1]
    sp = lax.axis_index("sp")
    tp = lax.axis_index("tp")
    chip = sp // 2
    core = sp % 2
    tp_x = (tp // 2) * 2 + (1 - tp % 2)
    tp_y = (1 - tp // 2) * 2 + tp % 2
    tp_d = (1 - tp // 2) * 2 + (1 - tp % 2)
    dev_x = (sp, tp_x)
    dev_y = (sp, tp_y)
    dev_s = (chip * 2 + (1 - core), tp)
    ks = list(range(n_chips))
    dev_z = [(flipped(chip, k) * 2 + core, tp) for k in ks]

    loads = []
    for i, (s, d) in enumerate(((ow_hbm, ow), (resid_hbm, resid), (wg_hbm.at[0], wg), (wu_hbm.at[0], wu), (wd_hbm.at[0], wd))):
        cp = pltpu.make_async_copy(s, d, local_sems.at[i])
        cp.start()
        loads.append(cp)

    count = [0]
    sent = []

    def remote(s, d, dev):
        i = count[0]
        count[0] += 1
        return pltpu.make_async_remote_copy(
            src_ref=s, dst_ref=d, send_sem=send_sems.at[i], recv_sem=recv_sems.at[i],
            device_id=dev, device_id_type=MESH,
        )

    def go(s, d, dev):
        cp = remote(s, d, dev)
        cp.start()
        sent.append(cp)
        return cp

    def cols(index, size):
        return pl.ds(pl.multiple_of(index * size, 128), size)

    barrier = pltpu.get_barrier_semaphore()
    peers = [dev_x, dev_y, dev_s] + dev_z[1:]
    for dev in peers:
        pl.semaphore_signal(barrier, inc=1, device_id=dev, device_id_type=MESH)
    other = jnp.where(core == 0, sp - 1, sp + 1)
    has_other = jnp.where(core == 0, chip > 0, chip < n_chips - 1)

    @pl.when(has_other)
    def _():
        pl.semaphore_signal(barrier, inc=1, device_id=(other, tp), device_id_type=MESH)

    product = (c_ref[...].astype(jnp.float32) * h_ref[...].astype(jnp.float32)).astype(jnp.bfloat16)
    ext[8:, :] = product.astype(jnp.float32)
    pl.semaphore_wait(barrier, len(peers) + has_other.astype(jnp.int32))

    edge = remote(ext.at[pl.ds(tok_rows, 8)], ext.at[pl.ds(0, 8)], (sp + 1, tp))

    @pl.when(sp < 2 * n_chips - 1)
    def _():
        edge.start()

    row_lane = lax.broadcasted_iota(jnp.int32, (1, tok_rows), 1)
    own_docs = docs_ref[:, cols(sp, tok_rows)].astype(jnp.float32)
    last_docs = docs_ref[
        :, pl.ds(pl.multiple_of(jnp.maximum(sp * tok_rows - 128, 0), 128), 128)
    ].astype(jnp.float32)
    one_back = jnp.where(row_lane == 0, last_docs[:, 127:], pltpu.roll(own_docs, 1, 1))
    two_back = jnp.where(
        row_lane == 0,
        last_docs[:, 126:127],
        jnp.where(row_lane == 1, last_docs[:, 127:], pltpu.roll(own_docs, 2, 1)),
    )
    position = row_lane + sp * tok_rows
    picks = pick_ref[...]
    odd = picks[0:1] % 2 == 1
    weight = weight_ref[...]
    facts = jnp.concatenate(
        [
            jnp.where((one_back == own_docs) & (position >= 1), 1.0, 0.0),
            jnp.where((two_back == own_docs) & (position >= 2), 1.0, 0.0),
            (picks[0:1] // 2).astype(jnp.float32),
            jnp.where(odd, weight[1:2], weight[0:1]),
            jnp.where(odd, weight[0:1], weight[1:2]),
            jnp.zeros((3, tok_rows), jnp.float32),
        ],
        axis=0,
    ).T
    def make_slots():
        lane = lax.broadcasted_iota(jnp.int32, (tok_rows, 128), 1)
        lane_f = lane.astype(jnp.float32)
        group = facts[:, 2:3]
        onehot = (group == lane_f).astype(jnp.float32)
        earlier = (
            lax.broadcasted_iota(jnp.int32, (tok_rows, tok_rows), 1)
            < lax.broadcasted_iota(jnp.int32, (tok_rows, tok_rows), 0)
        ).astype(jnp.float32).astype(jnp.bfloat16)
        before = jnp.dot(earlier, onehot.astype(jnp.bfloat16), preferred_element_type=jnp.float32)
        slot = jnp.sum(before * onehot, axis=1, keepdims=True)
        for k in ks:
            here = flipped(chip, k).astype(jnp.float32)
            hit = jnp.where((group == here) & (slot == lane_f) & (lane < capacity), 1.0, 0.0)
            pt[k] = hit.astype(jnp.bfloat16)
        parts = jnp.zeros((tok_rows, 128), jnp.float32)
        for j in range(2):
            w = facts[:, 3 + j : 4 + j]
            for i in range(3):
                piece = w.astype(jnp.bfloat16).astype(jnp.float32)
                parts = jnp.where(lane == 3 * j + i, piece, parts)
                w = w - piece
        parts = parts.astype(jnp.bfloat16)
        for k in ks:
            got = lax.dot_general(
                pt[k], parts, (((0,), (0,)), ((), ())), preferred_element_type=jnp.float32
            )
            wts_out[k] = got[:capacity].astype(jnp.bfloat16)
        wts[0] = wts_out[0]

    gain[...] = gain_ref[...].astype(jnp.float32)[None, :]

    taps = taps_ref[:, cols(tp, chans)].astype(jnp.float32)
    half_rows = tok_rows // 2

    def spread(buf, size, own_sends):
        mine = buf.at[:, cols(tp, size)]
        own_sends.append(go(mine, mine, dev_x))
        own_sends.append(go(mine, mine, dev_y))

    def relay(buf, size, sends):
        half = size // 2
        sends[1].wait_recv()
        part = buf.at[:, cols(tp_y * 2, half)]
        sends.append(go(part, part, dev_x))
        sends[0].wait_recv()
        part = buf.at[:, cols(tp_x * 2 + 1, half)]
        sends.append(go(part, part, dev_y))

    def convolve(h):
        at = h * half_rows
        conv = taps[0:1, :] * ext[8 + at : 8 + at + half_rows, :]
        for lag in (1, 2):
            conv = (
                conv
                + taps[lag : lag + 1, :]
                * ext[8 + at - lag : 8 + at - lag + half_rows, :]
                * facts[at : at + half_rows, lag - 1 : lag]
            )
        gate = b_ref[at : at + half_rows, :].astype(jnp.float32)
        cv[h, :, cols(tp, chans)] = (gate * conv).astype(jnp.bfloat16)
        spread(cv.at[h], chans, conv_sends[h])

    conv_sends = [[], []]
    convolve(1)

    @pl.when(sp > 0)
    def _():
        edge.wait_recv()

    @pl.when(sp == 0)
    def _():
        ext[0:8, :] = jnp.zeros((8, chans), jnp.float32)

    convolve(0)

    def proj(h, index):
        rows_ = pl.ds(pl.multiple_of(index * chans, 128), chans)
        return jnp.dot(cv[h, :, cols(index, chans)], ow[rows_, :], preferred_element_type=jnp.float32)

    make_slots()
    loads[0].wait()
    loads[1].wait()
    half_at = [pl.ds(h * half_rows, half_rows) for h in range(2)]
    relay(cv.at[1], chans, conv_sends[1])
    for h in (1, 0):
        acc[half_at[h], :] = resid[half_at[h], :].astype(jnp.float32) + proj(h, tp)
    acc[half_at[1], :] += proj(1, tp_x)
    acc[half_at[1], :] += proj(1, tp_y)
    relay(cv.at[0], chans, conv_sends[0])
    acc[half_at[0], :] += proj(0, tp_x)
    acc[half_at[0], :] += proj(0, tp_y)
    for h in (1, 0):
        conv_sends[h][2].wait_recv()
        conv_sends[h][3].wait_recv()
        stream[half_at[h], :] = (acc[half_at[h], :] + proj(h, tp_d)).astype(jnp.bfloat16)

    z_rows, z_wts = [None] * n_chips, [None] * n_chips
    mine = cols(tp, width)
    for k in [0] + ks[1:]:
        got = lax.dot_general(
            pt[k], stream[...], (((0,), (0,)), ((), ())), preferred_element_type=jnp.float32
        )[:capacity].astype(jnp.bfloat16)
        if k == 0:
            rows[0, 0, :, mine] = got
        else:
            rows_out[k] = got
            z_rows[k] = go(rows_out.at[k], rows.at[k, 0, :, mine], dev_z[k])
        if k == 0:
            row_sends = [[] for _ in ks]
            sis = [[] for _ in ks]
            first = True
            spread(rows.at[0, 0], width, row_sends[0])
            sis[0].append(go(rows.at[0, 0, :, mine], rows.at[0, 1, :, mine], dev_s))
    for k in ks[1:]:
        z_wts[k] = go(wts_out.at[k], wts.at[k], dev_z[k])

    def share(k, index, size):
        at = cols(index, size)
        sis[k].append(go(rows.at[k, 0, :, at], rows.at[k, 1, :, at], dev_s))

    def stage(k):
        if k > 0:
            z_rows[k].wait_recv()
            spread(rows.at[k, 0], width, row_sends[k])
            share(k, tp, width)

    def forward(k):
        relay(rows.at[k, 0], width, row_sends[k])
        share(k, tp_x, width)
        share(k, tp_y, width)

    def finish(k):
        row_sends[k][2].wait_recv()
        share(k, tp_d * 2, width // 2)
        row_sends[k][3].wait_recv()
        share(k, tp_d * 2 + 1, width // 2)

    hid_sends = [[] for _ in ks]

    def expand(k):
        for cp in sis[k]:
            cp.wait_recv()
        for p in range(2):
            def norm(r, carry, p=p):
                at = pl.ds(pl.multiple_of(r * 16, 16), 16)
                x = rows[k, p, at, :].astype(jnp.float32)
                ms = jnp.sum(x * x, axis=1, keepdims=True) / full
                inv = lax.rsqrt(ms + NORM_EPS)
                y = (x * inv * gain[...]).astype(jnp.bfloat16)
                normed[pl.ds(pl.multiple_of(p * capacity + r * 16, 16), 16), :] = y
                return carry
            lax.fori_loop(0, capacity // 16, norm, 0)
        if k == 0:
            loads[2].wait()
            loads[3].wait()

        def tile(n, carry):
            at = pl.ds(pl.multiple_of(n * 256, 256), 256)
            x = normed[...]
            g = jnp.dot(x, wg[:, at], preferred_element_type=jnp.float32)
            u = jnp.dot(x, wu[:, at], preferred_element_type=jnp.float32)
            h = (g / (1.0 + jnp.exp(-g)) * u).astype(jnp.bfloat16)
            hid[k, :, pl.ds(pl.multiple_of(tp * hid_cols + n * 256, 256), 256)] = h
            return carry

        lax.fori_loop(0, hid_cols // 256, tile, 0)

    def hid_send(k):
        spread(hid.at[k], hid_cols, hid_sends[k])

    def hid_forward(k):
        relay(hid.at[k], hid_cols, hid_sends[k])

    e_sends = [None] * n_chips
    late_loads = [loads[4]]
    z_back = [None] * n_chips

    def down(k):
        hid_sends[k][2].wait_recv()
        hid_sends[k][3].wait_recv()
        while late_loads:
            late_loads.pop().wait()

        def tile(n, carry):
            at = pl.ds(pl.multiple_of(n * 256, 256), 256)
            e = jnp.dot(hid[k], wd[:, at], preferred_element_type=jnp.float32).astype(jnp.bfloat16)
            e_own[k, :, at] = e[:capacity]
            e_send[k, :, at] = e[capacity:]
            return carry

        lax.fori_loop(0, width // 256, tile, 0)
        e_sends[k] = go(e_send.at[k], e_recv.at[k], dev_s)

    def combine(k):
        if k > 0:
            z_wts[k].wait_recv()
        w = wts[k].astype(jnp.float32)
        w_lane = lax.broadcasted_iota(jnp.int32, w.shape, 1)
        w_even = jnp.sum(jnp.where(w_lane < 3, w, 0.0), axis=1, keepdims=True)
        w_odd = jnp.sum(jnp.where((w_lane >= 3) & (w_lane < 6), w, 0.0), axis=1, keepdims=True)
        pick = core.astype(jnp.float32)
        w_mine = w_even * (1.0 - pick) + w_odd * pick
        w_other = w_odd * (1.0 - pick) + w_even * pick
        e_sends[k].wait_recv()
        f = (e_own[k].astype(jnp.float32) * w_mine + e_recv[k].astype(jnp.float32) * w_other).astype(jnp.bfloat16)
        if k == 0:
            back[0, 0:capacity, :] = f
        else:
            feed_out[k] = f
            z_back[k] = go(feed_out.at[k], back.at[k, pl.ds(0, capacity), :], dev_z[k])

    for k in ks:
        back[k, capacity:, :] = jnp.zeros((128 - capacity, width), jnp.bfloat16)

    steps = {
        "S": stage, "F": forward, "D": finish, "E": expand, "X": hid_send,
        "R": hid_forward, "W": down, "C": combine,
    }
    for step in PLAN.split():
        steps[step[0]](int(step[1:]))

    acc[...] = stream[...].astype(jnp.float32)
    for k in FINAL:
        if k > 0:
            z_back[k].wait_recv()
        acc[...] += jnp.dot(pt[k], back[k], preferred_element_type=jnp.float32)
    out_ref[...] = acc[...].astype(jnp.bfloat16)

    for cp in sent:
        cp.wait_send()

    @pl.when(sp < 2 * n_chips - 1)
    def _():
        edge.wait_send()


def fused(
    b_gate,
    c_gate,
    h_in,
    docs,
    conv_taps,
    out_weight,
    residual_in,
    norm_gain,
    expert_pick,
    route_weight,
    w_gate,
    w_up,
    w_down,
):
    tok_rows, chans = h_in.shape
    width = residual_in.shape[1]
    full = w_gate.shape[1]
    hid_cols = w_gate.shape[2]
    hid_full = w_down.shape[1]
    n_sp = lax.axis_size("sp")
    n_chips = n_sp // 2
    capacity = 5 * tok_rows // (2 * n_sp)
    n_copies = 9 + 2 * (n_chips - 1) + 14 * n_chips + n_chips - 1
    vmem = pl.BlockSpec(memory_space=pltpu.VMEM)
    hbm = pl.BlockSpec(memory_space=pl.ANY)
    bf16 = jnp.bfloat16
    return pl.pallas_call(
        functools.partial(fused_kernel, n_chips, capacity),
        out_shape=jax.ShapeDtypeStruct((tok_rows, width), bf16),
        in_specs=[vmem] * 8 + [hbm] * 5,
        out_specs=vmem,
        scratch_shapes=[
            pltpu.VMEM(residual_in.shape, bf16),
            pltpu.VMEM((1, full), jnp.float32),
            pltpu.VMEM(out_weight.shape, bf16),
            pltpu.VMEM(w_gate.shape[1:], bf16),
            pltpu.VMEM(w_up.shape[1:], bf16),
            pltpu.VMEM(w_down.shape[1:], bf16),
            pltpu.VMEM((tok_rows + 8, chans), jnp.float32),
            pltpu.VMEM((2, tok_rows // 2, out_weight.shape[0]), bf16),
            pltpu.VMEM((tok_rows, width), bf16),
            pltpu.VMEM((tok_rows, width), jnp.float32),
            pltpu.VMEM((n_chips, tok_rows, 128), bf16),
            pltpu.VMEM((n_chips, capacity, width), bf16),
            pltpu.VMEM((n_chips, capacity, 128), bf16),
            pltpu.VMEM((n_chips, 2, capacity, full), bf16),
            pltpu.VMEM((n_chips, capacity, 128), bf16),
            pltpu.VMEM((2 * capacity, full), bf16),
            pltpu.VMEM((n_chips, 2 * capacity, hid_full), bf16),
            pltpu.VMEM((n_chips, capacity, width), bf16),
            pltpu.VMEM((n_chips, capacity, width), bf16),
            pltpu.VMEM((n_chips, capacity, width), bf16),
            pltpu.VMEM((n_chips, capacity, width), bf16),
            pltpu.VMEM((n_chips, 128, width), bf16),
            pltpu.SemaphoreType.DMA((5,)),
            pltpu.SemaphoreType.DMA((n_copies,)),
            pltpu.SemaphoreType.DMA((n_copies,)),
        ],
        compiler_params=pltpu.CompilerParams(
            collective_id=0, has_side_effects=True, vmem_limit_bytes=56 * 1024 * 1024
        ),
    )(
        b_gate,
        c_gate,
        h_in,
        docs[None, :],
        expert_pick.T,
        route_weight.T,
        conv_taps,
        norm_gain,
        residual_in,
        out_weight,
        w_gate,
        w_up,
        w_down,
    )


def pairs_fit(mesh):
    n_sp, n_tp = mesh.shape["sp"], mesh.shape["tp"]
    return n_sp == GROUPS * TOP_K and TOP_K == 2 and n_tp == 4


def solution(mesh):
    return jax.shard_map(
        fused if pairs_fit(mesh) else general,
        mesh=mesh,
        in_specs=(
            P("sp", "tp"),
            P("sp", "tp"),
            P("sp", "tp"),
            P(),
            P(),
            P(None, "tp"),
            P("sp", "tp"),
            P(),
            P("sp", None),
            P("sp", None),
            P("sp", None, "tp"),
            P("sp", None, "tp"),
            P("sp", None, "tp"),
        ),
        out_specs=P("sp", "tp"),
        check_vma=False,
    )
```
